32 devices in a mesh: sp: 4 (over z), tp: 2 (over y), dp: 4 (over x, core).
Axes of the slice: x: 2, y: 2, z: 4, core: 2. Of those that a mesh axis runs over, the one named last changes fastest.
Arguments:
- latent: bfloat16 [5120, 3072], P(('dp', 'sp', 'tp')), parts along dimension 0, may hold values from -6 to 6
- condition: float32 [12288], P('dp'), parts along dimension 0, may hold values from -8 to 8
- ctx_condition: float32 [3072], replicated, may hold values from -8 to 8
- context: bfloat16 [512, 3072], P(('dp', 'sp')), parts along dimension 0, may hold values from -6 to 6
- mod_shift: bfloat16 [3072, 3072], P('sp', 'tp'), may hold values from -0.109375 to 0.109375
- mod_scale: bfloat16 [3072, 3072], P('sp', 'tp'), may hold values from -0.109375 to 0.109375
- mod_gate: bfloat16 [3072, 3072], P('sp', 'tp'), may hold values from -0.109375 to 0.109375
- norm_gain: float32 [3072], replicated, may hold values from 0.5 to 6
- w_query: bfloat16 [3072, 3072], P(None, 'tp'), may hold values from -0.109375 to 0.109375
- key_weight: bfloat16 [3072, 512], P(None, 'tp'), may hold values from -0.109375 to 0.109375
- value_weight: bfloat16 [3072, 512], P(None, 'tp'), may hold values from -0.109375 to 0.109375
- w_gate: bfloat16 [3072, 3072], P(None, 'tp'), may hold values from -0.109375 to 0.109375
- w_out: bfloat16 [3072, 3072], P('tp'), may hold values from -1.5 to 1.5
- sink_logit: float32 [48], P('tp'), may hold values from 4 to 7.5
Outputs:
- updated_latent: bfloat16 [5120, 3072], P(('dp', 'sp', 'tp')), parts along dimension 0
The draws below stay inside these ranges and needn't reach their ends.
There are 4 independent parts, one for each index of `dp`. The reference program is written for one: setup_inputs(seed, part) draws one part's arguments, and reference() takes and returns one part's arrays. A program takes and returns all parts, laid end to end along the dimension named above; an argument that names none is the same for every part. Nothing has to cross between parts.
All inputs are finite; a program needn't handle non-finite values.
Results may differ from the reference program's by a relative error of at most 0.02.
The reference program's roundings to bfloat16 on the way count: a program that leaves them out, or rounds other values in their place, can miss the bound.
Values may be sent and summed in bfloat16 or wider, within the bound.
A program may use at most 128 MiB of HBM per device.

```python
import math
import jax
import jax.numpy as jnp
from jax import lax

MODEL_WIDTH = 3072
HEAD_SIZE = 64
HQ = 48
KEY_VALUE_HEADS = 8
L_DEV = 320
WINDOW = 128
GRID_W = 64
SEQ = 1280
CTX = 128
N_TP = 2


def draw_norm_gain(key, part):
    return jax.random.uniform(key, (MODEL_WIDTH,), jnp.float32, 0.5, 1.5)


def block_scale(own_key, extent, split, low, largest):
    gain, own = 1.0, jax.random.fold_in(own_key, 6)
    for axis_at, shards_of in split:
        draws = jnp.exp(jax.random.uniform(jax.random.fold_in(own, axis_at), (shards_of,), jnp.float32, low / len(split), largest / len(split)))
        gain = gain * jnp.repeat(draws, extent[axis_at] // shards_of).reshape([-1 if axis == axis_at else 1 for axis in range(len(extent))])
    return gain


def scatter_about(stream_key, shape, spread, most, cuts=(), held_as=jnp.bfloat16):
    gain = block_scale(stream_key, shape, cuts, -0.22, 0.18) if cuts else 1.0
    values = jax.random.normal(stream_key, shape, jnp.float32) * spread * gain
    return jnp.minimum(jnp.maximum(values, -most), most).astype(held_as)


def setup_inputs(seed: int = 0, part: int = 0) -> dict:
    streams_of = jax.random.split(jax.random.key(seed), 15)
    part_keys = jax.random.split(jax.random.fold_in(streams_of[14], part), 15)
    return {
        "latent": scatter_about(part_keys[0], (SEQ, MODEL_WIDTH), 1.0, 6.0, ((0, 8),)),
        "condition": scatter_about(part_keys[1], (MODEL_WIDTH,), 1.5, 8.0, (), jnp.float32),
        "ctx_condition": scatter_about(streams_of[2], (MODEL_WIDTH,), 1.5, 8.0, (), jnp.float32),
        "context": scatter_about(part_keys[3], (CTX, MODEL_WIDTH), 1.0, 6.0, ((0, 4),)),
        "mod_shift": scatter_about(streams_of[4], (MODEL_WIDTH, MODEL_WIDTH), MODEL_WIDTH ** -0.5, 0.109375, ((0, 4), (1, 2))),
        "mod_scale": scatter_about(streams_of[5], (MODEL_WIDTH, MODEL_WIDTH), MODEL_WIDTH ** -0.5, 0.109375, ((0, 4), (1, 2))),
        "mod_gate": scatter_about(streams_of[6], (MODEL_WIDTH, MODEL_WIDTH), MODEL_WIDTH ** -0.5, 0.109375, ((0, 4), (1, 2))),
        "norm_gain": draw_norm_gain(jax.random.fold_in(streams_of[14], 71), part),
        "w_query": scatter_about(streams_of[8], (MODEL_WIDTH, HQ * HEAD_SIZE), MODEL_WIDTH ** -0.5, 0.109375, ((1, 2),)),
        "key_weight": scatter_about(streams_of[9], (MODEL_WIDTH, KEY_VALUE_HEADS * HEAD_SIZE), MODEL_WIDTH ** -0.5, 0.109375, ((1, 2),)),
        "value_weight": scatter_about(streams_of[10], (MODEL_WIDTH, KEY_VALUE_HEADS * HEAD_SIZE), MODEL_WIDTH ** -0.5, 0.109375, ((1, 2),)),
        "w_gate": scatter_about(streams_of[11], (MODEL_WIDTH, HQ * HEAD_SIZE), MODEL_WIDTH ** -0.5, 0.109375, ((1, 2),)),
        "w_out": scatter_about(streams_of[12], (HQ * HEAD_SIZE, MODEL_WIDTH), 16 ** -0.5, 1.5, ((0, 2),)),
        "sink_logit": jnp.clip(4.0 + 3.5 * jax.random.uniform(streams_of[13], (HQ,), jnp.float32) ** block_scale(streams_of[13], (HQ,), ((0, 2),), -0.2, 0.2), 4.0, 7.5),
    }


NORM_EPS = 1e-06
MASK_VALUE = -1e+30

def modulate(row_data, gain_vec, shift_vec, scale_vec):
    values = row_data.astype(jnp.float32)
    inverse = lax.rsqrt(lax.optimization_barrier(jnp.mean(values * values, axis=-1, keepdims=True)) + NORM_EPS)
    return (values * inverse * gain_vec * (1.0 + scale_vec) + shift_vec).astype(jnp.bfloat16)

def rotate(projected, positions):
    row_count = projected.shape[0]
    head_count = projected.shape[1] // HEAD_SIZE
    quarter = HEAD_SIZE // 4
    half_dim = HEAD_SIZE // 2
    inverse = jnp.exp(-math.log(10000.0) * jnp.arange(quarter, dtype=jnp.float32) / quarter)
    grid_row = (positions // GRID_W).astype(jnp.float32)
    mesh_column = (positions % GRID_W).astype(jnp.float32)
    angles = jnp.concatenate([grid_row[:, None] * inverse, mesh_column[:, None] * inverse], axis=1)
    cosine = jnp.cos(angles)[:, None, :]
    sine_table = jnp.sin(angles)[:, None, :]
    shaped = projected.reshape(row_count, head_count, HEAD_SIZE)
    first_half = shaped[..., :half_dim]
    second = shaped[..., half_dim:]
    turned = jnp.concatenate([first_half * cosine - second * sine_table, second * cosine + first_half * sine_table], axis=-1)
    return turned.reshape(row_count, head_count * HEAD_SIZE)

def attend(queries, key_rows, value_rows, ctx_keys, ctx_values, sink_logit, q_begin, k_begin, seq_total):
    row_count = queries.shape[0]
    key_count = key_rows.shape[0]
    ctx_count = ctx_keys.shape[0]
    kv_heads = key_rows.shape[1] // HEAD_SIZE
    head_count = queries.shape[1] // HEAD_SIZE
    group_size = head_count // kv_heads
    factor = 1.0 / math.sqrt(HEAD_SIZE)
    q_heads = queries.astype(jnp.float32).reshape(row_count, kv_heads, group_size, HEAD_SIZE)
    k_heads = key_rows.astype(jnp.float32).reshape(key_count, kv_heads, HEAD_SIZE)
    v_heads = value_rows.astype(jnp.float32).reshape(key_count, kv_heads, HEAD_SIZE)
    ck_heads = ctx_keys.astype(jnp.float32).reshape(ctx_count, kv_heads, HEAD_SIZE)
    cv_heads = ctx_values.astype(jnp.float32).reshape(ctx_count, kv_heads, HEAD_SIZE)
    near_scores = jnp.einsum('qkgd,skd->kgqs', q_heads, k_heads) * factor
    q_pos = q_begin + jnp.arange(row_count, dtype=jnp.int32)
    k_pos = k_begin + jnp.arange(key_count, dtype=jnp.int32)
    in_window = (jnp.abs(q_pos[:, None] - k_pos[None, :]) <= WINDOW) & ((k_pos >= 0) & (k_pos < seq_total))[None, :]
    near_scores = jnp.where(in_window, near_scores, MASK_VALUE)
    ctx_scores = jnp.einsum('qkgd,skd->kgqs', q_heads, ck_heads) * factor
    sink_score = sink_logit.astype(jnp.float32).reshape(kv_heads, group_size)[:, :, None, None]
    peak_score = jnp.maximum(jnp.maximum(lax.optimization_barrier(jnp.max(near_scores, axis=-1, keepdims=True)), lax.optimization_barrier(jnp.max(ctx_scores, axis=-1, keepdims=True))), sink_score)
    near_exp = jnp.exp(near_scores - peak_score)
    ctx_exp = jnp.exp(ctx_scores - peak_score)
    softmax_denominator = lax.optimization_barrier(jnp.sum(near_exp, axis=-1, keepdims=True)) + lax.optimization_barrier(jnp.sum(ctx_exp, axis=-1, keepdims=True)) + jnp.exp(sink_score - peak_score)
    near_weights = (near_exp / softmax_denominator).astype(jnp.bfloat16)
    ctx_weights = (ctx_exp / softmax_denominator).astype(jnp.bfloat16)
    result = jnp.einsum('kgqs,skd->qkgd', near_weights.astype(jnp.float32), v_heads)
    result = result + jnp.einsum('kgqs,skd->qkgd', ctx_weights.astype(jnp.float32), cv_heads)
    return result.reshape(row_count, head_count * HEAD_SIZE)

def project_vec(vector, matrix):
    return jnp.dot(vector[None, :], matrix, preferred_element_type=jnp.float32)[0]

def reference(latent, condition, ctx_condition, context, mod_shift, mod_scale, mod_gate, norm_gain, w_query, key_weight, value_weight, w_gate, w_out, sink_logit):
    cond_act = jax.nn.silu(condition.astype(jnp.float32)).astype(jnp.bfloat16)
    ctx_act = jax.nn.silu(ctx_condition.astype(jnp.float32)).astype(jnp.bfloat16)
    lat_shift = project_vec(cond_act, mod_shift)
    lat_scale = project_vec(cond_act, mod_scale)
    lat_gate = project_vec(cond_act, mod_gate)
    ctx_shift = project_vec(ctx_act, mod_shift)
    ctx_scale = project_vec(ctx_act, mod_scale)
    hidden = modulate(latent, norm_gain, lat_shift, lat_scale)
    ctx_hidden = modulate(context, norm_gain, ctx_shift, ctx_scale)
    seq_total = latent.shape[0]
    positions = jnp.arange(seq_total, dtype=jnp.int32)
    queries = rotate(jnp.dot(hidden, w_query, preferred_element_type=jnp.float32), positions).astype(jnp.bfloat16)
    key_rows = rotate(jnp.dot(hidden, key_weight, preferred_element_type=jnp.float32), positions).astype(jnp.bfloat16)
    value_rows = jnp.dot(hidden, value_weight, preferred_element_type=jnp.float32).astype(jnp.bfloat16)
    gate_proj = jnp.dot(hidden, w_gate, preferred_element_type=jnp.float32).astype(jnp.bfloat16)
    ctx_keys = jnp.dot(ctx_hidden, key_weight, preferred_element_type=jnp.float32).astype(jnp.bfloat16)
    ctx_values = jnp.dot(ctx_hidden, value_weight, preferred_element_type=jnp.float32).astype(jnp.bfloat16)
    key_pad = jnp.pad(key_rows, ((WINDOW, WINDOW), (0, 0)))
    value_pad = jnp.pad(value_rows, ((WINDOW, WINDOW), (0, 0)))
    key_span = L_DEV + 2 * WINDOW

    def one_block(block_index):
        begin_row = (block_index * L_DEV).astype(jnp.int32)
        q_block = lax.dynamic_slice_in_dim(queries, begin_row, L_DEV, 0)
        k_block = lax.dynamic_slice_in_dim(key_pad, begin_row, key_span, 0)
        v_block = lax.dynamic_slice_in_dim(value_pad, begin_row, key_span, 0)
        return attend(q_block, k_block, v_block, ctx_keys, ctx_values, sink_logit, begin_row, begin_row - WINDOW, seq_total)
    blocks = lax.map(one_block, jnp.arange(seq_total // L_DEV, dtype=jnp.int32))
    attended = blocks.reshape(seq_total, queries.shape[1])
    mixed = (attended * jax.nn.silu(gate_proj.astype(jnp.float32))).astype(jnp.bfloat16)
    group_size = w_out.shape[0] // N_TP
    branch = jnp.zeros(latent.shape, jnp.float32)
    for group_index in range(N_TP):
        lower = group_index * group_size
        partial_term = jnp.dot(mixed[:, lower:lower + group_size], w_out[lower:lower + group_size], preferred_element_type=jnp.float32)
        branch = branch + lax.optimization_barrier(partial_term.astype(jnp.bfloat16)).astype(jnp.float32)
    return (latent.astype(jnp.float32) + lat_gate * branch).astype(jnp.bfloat16)
```

```python
import functools
import math

import jax
import jax.numpy as jnp
from jax import lax
from jax.experimental import pallas as pl
from jax.experimental.pallas import tpu as pltpu
from jax.sharding import PartitionSpec as P

HEAD_SIZE = 64
WINDOW = 128
GRID_W = 64


NORM_EPS = 1e-06
MASK_VALUE = -1e30


def with_halo(block, sides, width):
    for axis, dim in sides:
        count = lax.axis_size(axis)
        forward = [(i, i + 1) for i in range(count - 1)]
        backward = [(target, source) for source, target in forward]
        low = lax.ppermute(
            lax.slice_in_dim(block, block.shape[dim] - width, None, axis=dim), axis, forward
        )
        high = lax.ppermute(lax.slice_in_dim(block, 0, width, axis=dim), axis, backward)
        block = jnp.concatenate([low, block, high], axis=dim)
    return block


def modulate(row_data, gain_vec, shift_vec, scale_vec):
    values = row_data.astype(jnp.float32)
    inverse = lax.rsqrt(jnp.mean(values * values, axis=-1, keepdims=True) + NORM_EPS)
    return (values * inverse * gain_vec * (1.0 + scale_vec) + shift_vec).astype(jnp.bfloat16)


def rotate(projected, positions):
    row_count = projected.shape[0]
    head_count = projected.shape[1] // HEAD_SIZE
    quarter = HEAD_SIZE // 4
    half_dim = HEAD_SIZE // 2
    inverse = jnp.exp(-math.log(10000.0) * jnp.arange(quarter, dtype=jnp.float32) / quarter)
    grid_row = (positions // GRID_W).astype(jnp.float32)
    mesh_column = (positions % GRID_W).astype(jnp.float32)
    angles = jnp.concatenate([grid_row[:, None] * inverse, mesh_column[:, None] * inverse], axis=1)
    cosine = jnp.cos(angles)[:, None, :]
    sine_table = jnp.sin(angles)[:, None, :]
    shaped = projected.reshape(row_count, head_count, HEAD_SIZE)
    first_half = shaped[..., :half_dim]
    second = shaped[..., half_dim:]
    turned = jnp.concatenate(
        [first_half * cosine - second * sine_table, second * cosine + first_half * sine_table],
        axis=-1,
    )
    return turned.reshape(row_count, head_count * HEAD_SIZE)


def attend(
    queries, key_rows, value_rows, ctx_keys, ctx_values, sink_logit, q_begin, k_begin, seq_total
):
    row_count = queries.shape[0]
    key_count = key_rows.shape[0]
    ctx_count = ctx_keys.shape[0]
    kv_heads = key_rows.shape[1] // HEAD_SIZE
    head_count = queries.shape[1] // HEAD_SIZE
    group_size = head_count // kv_heads
    factor = 1.0 / math.sqrt(HEAD_SIZE)
    q_heads = queries.reshape(row_count, kv_heads, group_size, HEAD_SIZE)
    k_heads = key_rows.reshape(key_count, kv_heads, HEAD_SIZE)
    v_heads = value_rows.reshape(key_count, kv_heads, HEAD_SIZE)
    ck_heads = ctx_keys.reshape(ctx_count, kv_heads, HEAD_SIZE)
    cv_heads = ctx_values.reshape(ctx_count, kv_heads, HEAD_SIZE)
    near_scores = (
        jnp.einsum("qkgd,skd->kgqs", q_heads, k_heads, preferred_element_type=jnp.float32) * factor
    )
    q_pos = q_begin + jnp.arange(row_count, dtype=jnp.int32)
    k_pos = k_begin + jnp.arange(key_count, dtype=jnp.int32)
    in_window = (jnp.abs(q_pos[:, None] - k_pos[None, :]) <= WINDOW) & (
        (k_pos >= 0) & (k_pos < seq_total)
    )[None, :]
    near_scores = jnp.where(in_window, near_scores, MASK_VALUE)
    ctx_scores = (
        jnp.einsum("qkgd,skd->kgqs", q_heads, ck_heads, preferred_element_type=jnp.float32) * factor
    )
    sink_score = sink_logit.reshape(kv_heads, group_size)[:, :, None, None]
    peak_score = jnp.maximum(
        jnp.maximum(
            jnp.max(near_scores, axis=-1, keepdims=True),
            jnp.max(ctx_scores, axis=-1, keepdims=True),
        ),
        sink_score,
    )
    near_exp = jnp.exp(near_scores - peak_score)
    ctx_exp = jnp.exp(ctx_scores - peak_score)
    softmax_denominator = (
        jnp.sum(near_exp, axis=-1, keepdims=True)
        + jnp.sum(ctx_exp, axis=-1, keepdims=True)
        + jnp.exp(sink_score - peak_score)
    )
    near_weights = (near_exp / softmax_denominator).astype(jnp.bfloat16)
    ctx_weights = (ctx_exp / softmax_denominator).astype(jnp.bfloat16)
    result = jnp.einsum("kgqs,skd->qkgd", near_weights, v_heads, preferred_element_type=jnp.float32)
    result = result + jnp.einsum(
        "kgqs,skd->qkgd", ctx_weights, cv_heads, preferred_element_type=jnp.float32
    )
    return result.reshape(row_count, head_count * HEAD_SIZE)


def shards(
    latent,
    condition,
    ctx_condition,
    context,
    mod_shift,
    mod_scale,
    mod_gate,
    norm_gain,
    w_query,
    key_weight,
    value_weight,
    w_gate,
    w_out,
    sink_logit,
):
    sp_count = lax.axis_size("sp")
    sp_rank = lax.axis_index("sp")
    mod_rows = mod_shift.shape[0]
    cond_act = jax.nn.silu(condition).astype(jnp.bfloat16)
    ctx_act = jax.nn.silu(ctx_condition).astype(jnp.bfloat16)
    first_row = sp_rank * mod_rows
    lat_piece = lax.dynamic_slice_in_dim(cond_act, first_row, mod_rows, 0)
    ctx_piece = lax.dynamic_slice_in_dim(ctx_act, first_row, mod_rows, 0)
    both_conds = jnp.stack([lat_piece, ctx_piece])
    partial_value = jnp.concatenate(
        [
            jnp.dot(both_conds, mod_shift, preferred_element_type=jnp.float32),
            jnp.dot(both_conds, mod_scale, preferred_element_type=jnp.float32),
            jnp.dot(lat_piece[None, :], mod_gate, preferred_element_type=jnp.float32),
        ],
        axis=0,
    )
    summed = lax.psum(partial_value, "sp")
    vectors = lax.all_gather(summed, "tp", axis=1, tiled=True)
    lat_shift = vectors[0]
    ctx_shift = vectors[1]
    lat_scale = vectors[2]
    ctx_scale = vectors[3]
    lat_gate = vectors[4]
    hidden = modulate(latent, norm_gain, lat_shift, lat_scale)
    ctx_hidden = modulate(context, norm_gain, ctx_shift, ctx_scale)
    kv_width = key_weight.shape[1]
    q_width = w_query.shape[1]
    ctx_pair = jnp.concatenate(
        [
            jnp.dot(ctx_hidden, key_weight, preferred_element_type=jnp.float32).astype(
                jnp.bfloat16
            ),
            jnp.dot(ctx_hidden, value_weight, preferred_element_type=jnp.float32).astype(
                jnp.bfloat16
            ),
        ],
        axis=1,
    )
    ctx_all = lax.all_gather(ctx_pair, "sp", axis=0, tiled=True)
    row_piece = lax.all_gather(hidden, "tp", axis=0, tiled=True)
    projected = jnp.concatenate(
        [
            jnp.dot(row_piece, w_query, preferred_element_type=jnp.float32),
            jnp.dot(row_piece, key_weight, preferred_element_type=jnp.float32),
            jnp.dot(row_piece, value_weight, preferred_element_type=jnp.float32),
            jnp.dot(row_piece, w_gate, preferred_element_type=jnp.float32),
        ],
        axis=1,
    )
    block_rows = projected.shape[0]
    q_begin = sp_rank * block_rows
    positions = q_begin + jnp.arange(block_rows, dtype=jnp.int32)
    queries = rotate(projected[:, :q_width], positions).astype(jnp.bfloat16)
    key_rows = rotate(projected[:, q_width : q_width + kv_width], positions).astype(jnp.bfloat16)
    value_rows = projected[:, q_width + kv_width : q_width + 2 * kv_width].astype(jnp.bfloat16)
    gate_proj = projected[:, q_width + 2 * kv_width :].astype(jnp.bfloat16)
    key_value = jnp.concatenate([key_rows, value_rows], axis=1)
    padded = with_halo(key_value, (("sp", 0),), WINDOW)
    attended = attend(
        queries,
        padded[:, :kv_width],
        padded[:, kv_width:],
        ctx_all[:, :kv_width],
        ctx_all[:, kv_width:],
        sink_logit,
        q_begin,
        q_begin - WINDOW,
        block_rows * sp_count,
    )
    mixed = (attended * jax.nn.silu(gate_proj.astype(jnp.float32))).astype(jnp.bfloat16)
    branch = lax.psum_scatter(
        jnp.dot(mixed, w_out, preferred_element_type=jnp.float32).astype(jnp.bfloat16),
        "tp",
        scatter_dimension=0,
        tiled=True,
    ).astype(jnp.float32)
    return (latent.astype(jnp.float32) + lat_gate * branch).astype(jnp.bfloat16)


MESH = pl.DeviceIdType.MESH
LANES = 128
Q_ROWS = 80
PIECES = 4
F32 = jnp.float32
BF16 = jnp.bfloat16


def block_kernel(
    sp_count,
    latent_hbm,
    cond_ref,
    ctx_cond_ref,
    context_hbm,
    ms_hbm,
    mc_hbm,
    mg_hbm,
    gain_ref,
    wq_hbm,
    wk_hbm,
    wv_hbm,
    wg_hbm,
    wo_hbm,
    sink_ref,
    cos_ref,
    sin_ref,
    out_ref,
    lat,
    ctx_rows,
    mods,
    wq,
    wk,
    wv,
    wg,
    wo,
    part,
    part_in,
    vecs,
    modv,
    hid,
    ctx_hid,
    qbuf,
    gbuf,
    kv,
    ctx_kv,
    mixed,
    bsend,
    brecv,
    local_sem,
    lat_sem,
    part_sem,
    vec_sem,
    ctx_sem,
    halo_sem,
    out_sem,
):
    rank = lax.axis_index("sp")
    side = lax.axis_index("tp")
    other = 1 - side
    own_rows, width = latent_hbm.shape
    block = 2 * own_rows
    mod_rows, mod_cols = ms_hbm.shape
    kv_width = wk.shape[1]
    q_width = wq.shape[1]
    ctx_own = context_hbm.shape[0]
    ctx_total = ctx_own * sp_count
    kv_heads = kv_width // HEAD_SIZE
    pairs = q_width // LANES // kv_heads
    keys = Q_ROWS + 2 * WINDOW
    span = -(-keys // LANES) * LANES
    total_keys = span + ctx_total
    piece = width // PIECES
    chunks_own = own_rows // Q_ROWS
    low_end = WINDOW + block

    def load(src, dst, index):
        return pltpu.make_async_copy(src, dst, local_sem.at[index])

    own_at = pl.multiple_of(side * own_rows, 16)
    far_at = pl.multiple_of(other * own_rows, 16)
    loads = [
        load(ms_hbm, mods.at[0], 0),
        load(mc_hbm, mods.at[1], 1),
        load(mg_hbm, mods.at[2], 2),
        load(latent_hbm, lat.at[pl.ds(own_at, own_rows)], 3),
        load(context_hbm, ctx_rows, 4),
        load(wk_hbm, wk, 5),
        load(wv_hbm, wv, 6),
        load(wq_hbm, wq, 7),
        load(wg_hbm, wg, 8),
        load(wo_hbm, wo, 9),
    ]
    for copy in loads:
        copy.start()

    barrier = pltpu.get_barrier_semaphore()
    pl.semaphore_signal(barrier, inc=1, device_id={"tp": other}, device_id_type=MESH)
    for step in range(1, sp_count):
        peer = lax.rem(rank + step, sp_count)
        pl.semaphore_signal(barrier, inc=1, device_id={"sp": peer}, device_id_type=MESH)
    pl.semaphore_wait(barrier, sp_count)

    def lat_copy(c):
        return pltpu.make_async_remote_copy(
            src_ref=latent_hbm.at[pl.ds(c * Q_ROWS, Q_ROWS)],
            dst_ref=lat.at[pl.ds(pl.multiple_of(own_at + c * Q_ROWS, 16), Q_ROWS)],
            send_sem=lat_sem.at[0, c],
            recv_sem=lat_sem.at[1, c],
            device_id={"tp": other},
            device_id_type=MESH,
        )

    lat_copies = [lat_copy(c) for c in range(chunks_own)]
    lat_copies[0].start()

    @pl.when(rank == 0)
    def _():
        kv[0:WINDOW, :] = jnp.zeros((WINDOW, 2 * kv_width), BF16)

    @pl.when(rank == sp_count - 1)
    def _():
        kv[low_end : low_end + WINDOW, :] = jnp.zeros((WINDOW, 2 * kv_width), BF16)

    first = pl.multiple_of(rank * mod_rows, LANES)
    lat_c = cond_ref[:, pl.ds(first, mod_rows)]
    ctx_c = ctx_cond_ref[:, pl.ds(first, mod_rows)]
    row_id = lax.broadcasted_iota(jnp.int32, (16, mod_rows), 0)
    both = jnp.where(row_id == 0, lat_c, ctx_c)
    both = (both / (1.0 + jnp.exp(-both))).astype(BF16)
    tile = mod_cols // 3
    for m in range(3):
        loads[m].wait()
        for t in range(3):
            cols = slice(t * tile, (t + 1) * tile)
            prod = jnp.dot(both, mods[m, :, cols], preferred_element_type=F32)
            part[2 * m : 2 * m + 2, cols] = prod[0:2, :]
    part[6:8, :] = jnp.zeros((2, mod_cols), F32)

    part_copies = []
    for step in range(1, sp_count):
        peer = lax.rem(rank + step, sp_count)
        copy = pltpu.make_async_remote_copy(
            src_ref=part,
            dst_ref=part_in.at[step - 1],
            send_sem=part_sem.at[0, step - 1],
            recv_sem=part_sem.at[1, step - 1],
            device_id={"sp": peer},
            device_id_type=MESH,
        )
        copy.start()
        part_copies.append(copy)
    for copy in part_copies:
        copy.wait()
    summed = part[...]
    for step in range(sp_count - 1):
        summed = summed + part_in[step]
    vecs[side] = summed
    vec_copy = pltpu.make_async_remote_copy(
        src_ref=vecs.at[side],
        dst_ref=vecs.at[side],
        send_sem=vec_sem.at[0],
        recv_sem=vec_sem.at[1],
        device_id={"tp": other},
        device_id_type=MESH,
    )
    vec_copy.start()
    for copy in lat_copies[1:]:
        copy.start()
    vec_copy.wait()
    for h in range(2):
        cols = slice(h * mod_cols, (h + 1) * mod_cols)
        gain = gain_ref[:, cols]
        modv[0:1, cols] = gain * (1.0 + vecs[h, 2:3, :])
        modv[1:2, cols] = vecs[h, 0:1, :]
        modv[2:3, cols] = gain * (1.0 + vecs[h, 3:4, :])
        modv[3:4, cols] = vecs[h, 1:2, :]
        modv[4:5, cols] = vecs[h, 4:5, :]

    def modulate_rows(src, dst, begin, count, which):
        def body(i, carry):
            rows = pl.ds(pl.multiple_of(begin + i * 16, 16), 16)
            values = src[rows, :].astype(F32)
            mean = jnp.sum(values * values, axis=-1, keepdims=True) * (1.0 / width)
            inverse = lax.rsqrt(mean + NORM_EPS)
            scaled = values * inverse * modv[which : which + 1, :] + modv[which + 1 : which + 2, :]
            dst[rows, :] = scaled.astype(BF16)
            return carry

        lax.fori_loop(0, count // 16, body, 0)

    def turn(values, rows, factor):
        lane = lax.broadcasted_iota(jnp.int32, values.shape, 1)
        half = HEAD_SIZE // 2
        ahead = pltpu.roll(values, LANES - half, 1)
        behind = pltpu.roll(values, half, 1)
        swapped = jnp.where(lane % HEAD_SIZE < half, ahead, behind)
        turned = values * cos_ref[rows, :] + swapped * sin_ref[rows, :]
        return turned * factor

    def project_kv(begin):
        rows = pl.ds(begin, own_rows)
        into = pl.ds(pl.multiple_of(begin + WINDOW, 16), own_rows)
        x = hid[rows, :]
        k = jnp.dot(x, wk[...], preferred_element_type=F32)
        for c in range(kv_width // LANES):
            cols = slice(c * LANES, (c + 1) * LANES)
            kv[into, cols] = turn(k[:, cols], rows, 1.0).astype(BF16)
        v = jnp.dot(x, wv[...], preferred_element_type=F32)
        kv[into, kv_width : 2 * kv_width] = v.astype(BF16)

    step_cols = 2 * LANES

    def project_q(begin):
        rows = pl.ds(begin, own_rows)
        factor = 1.0 / math.sqrt(HEAD_SIZE)

        def body(t, carry):
            at = pl.multiple_of(t * step_cols, step_cols)
            y = jnp.dot(hid[rows, :], wq[:, pl.ds(at, step_cols)], preferred_element_type=F32)
            for c in range(2):
                cols = pl.ds(pl.multiple_of(at + c * LANES, LANES), LANES)
                part_y = y[:, c * LANES : (c + 1) * LANES]
                qbuf[rows, cols] = turn(part_y, rows, factor).astype(BF16)
            return carry

        lax.fori_loop(0, q_width // step_cols, body, 0)

    def project_g(begin):
        rows = pl.ds(begin, own_rows)

        def body(t, carry):
            cols = pl.ds(pl.multiple_of(t * step_cols, step_cols), step_cols)
            y = jnp.dot(hid[rows, :], wg[:, cols], preferred_element_type=F32)
            gbuf[rows, cols] = y.astype(BF16)
            return carry

        lax.fori_loop(0, q_width // step_cols, body, 0)

    loads[4].wait()
    modulate_rows(ctx_rows, ctx_hid, 0, ctx_own, 2)
    loads[5].wait()
    loads[6].wait()
    ctx_at = pl.ds(pl.multiple_of(rank * ctx_own, 16), ctx_own)
    xc = ctx_hid[...]
    ctx_kv[ctx_at, 0:kv_width] = jnp.dot(xc, wk[...], preferred_element_type=F32).astype(BF16)
    ctx_kv[ctx_at, kv_width : 2 * kv_width] = jnp.dot(
        xc, wv[...], preferred_element_type=F32
    ).astype(BF16)
    ctx_copies = []
    for step in range(1, sp_count):
        peer = lax.rem(rank + step, sp_count)
        copy = pltpu.make_async_remote_copy(
            src_ref=ctx_kv.at[ctx_at],
            dst_ref=ctx_kv.at[ctx_at],
            send_sem=ctx_sem.at[0, step - 1],
            recv_sem=ctx_sem.at[1, step - 1],
            device_id={"sp": peer},
            device_id_type=MESH,
        )
        copy.start()
        ctx_copies.append(copy)

    def halo(src_at, dst_at, index, target):
        return pltpu.make_async_remote_copy(
            src_ref=kv.at[pl.ds(pl.multiple_of(src_at, 16), WINDOW)],
            dst_ref=kv.at[pl.ds(pl.multiple_of(dst_at, 16), WINDOW)],
            send_sem=halo_sem.at[0, index],
            recv_sem=halo_sem.at[1, index],
            device_id={"sp": target},
            device_id_type=MESH,
        )

    early_to = rank - 1 + 2 * side
    late_to = rank + 1 - 2 * side
    has_early_to = (early_to >= 0) & (early_to < sp_count)
    has_late_to = (late_to >= 0) & (late_to < sp_count)
    early = halo(WINDOW + side * (block - WINDOW), other * low_end, 0, early_to)
    late = halo(WINDOW + other * (block - WINDOW), side * low_end, 1, late_to)

    loads[3].wait()
    modulate_rows(lat, hid, own_at, own_rows, 0)
    project_kv(own_at)

    @pl.when(has_early_to)
    def _():
        early.start()

    loads[7].wait()
    project_q(own_at)
    loads[8].wait()
    project_g(own_at)

    for c in range(chunks_own):
        lat_copies[c].wait()
        modulate_rows(lat, hid, pl.multiple_of(far_at + c * Q_ROWS, 16), Q_ROWS, 0)
    project_kv(far_at)

    @pl.when(has_late_to)
    def _():
        late.start()

    project_q(far_at)
    project_g(far_at)
    for copy in ctx_copies:
        copy.wait()

    @pl.when(has_late_to)
    def _():
        early.wait_recv()

    loads[9].wait()

    def attend_rows(begin):
        rows = pl.ds(begin, Q_ROWS)
        i = lax.broadcasted_iota(jnp.int32, (Q_ROWS, span), 0)
        j = lax.broadcasted_iota(jnp.int32, (Q_ROWS, span), 1)
        offset = j - i
        k_pos = rank * block + begin - WINDOW + j
        allowed = (offset >= 0) & (offset <= 2 * WINDOW) & (k_pos >= 0)
        allowed = allowed & (k_pos < block * sp_count)
        bias = jnp.where(allowed, 0.0, MASK_VALUE)
        lane = lax.broadcasted_iota(jnp.int32, (total_keys, LANES), 1)
        low_lane = lane < HEAD_SIZE
        filler = jnp.zeros((span - keys, LANES), BF16)
        out_low = lax.broadcasted_iota(jnp.int32, (Q_ROWS, LANES), 1) < HEAD_SIZE

        def both_heads(at):
            cols = slice(at, at + LANES)
            tile_kv = jnp.concatenate(
                [kv[pl.ds(begin, keys), cols], filler, ctx_kv[:, cols]], axis=0
            ).astype(F32)
            turned = pltpu.roll(tile_kv, HEAD_SIZE, 1)
            even = jnp.concatenate(
                [jnp.where(low_lane, tile_kv, 0.0), jnp.where(low_lane, 0.0, turned)], axis=0
            )
            odd = jnp.concatenate(
                [jnp.where(low_lane, turned, 0.0), jnp.where(low_lane, 0.0, tile_kv)], axis=0
            )
            return even.astype(BF16), odd.astype(BF16)

        for tile_id in range(kv_heads // 2):
            k_two = both_heads(tile_id * LANES)
            v_two = both_heads(kv_width + tile_id * LANES)
            for parity in range(2):
                head = 2 * tile_id + parity
                k_wide = k_two[parity]
                v_wide = v_two[parity]
                base = head * pairs
                for p in range(pairs):
                    cols = slice((base + p) * LANES, (base + p + 1) * LANES)
                    scores = lax.dot_general(
                        qbuf[rows, cols],
                        k_wide,
                        (((1,), (1,)), ((), ())),
                        preferred_element_type=F32,
                    )
                    exps = []
                    scale = []
                    for h in range(2):
                        sink = sink_ref[2 * (base + p) + h]
                        near = scores[:, h * total_keys : h * total_keys + span] + bias
                        far = scores[:, h * total_keys + span : (h + 1) * total_keys]
                        peak = jnp.maximum(
                            jnp.max(near, axis=-1, keepdims=True),
                            jnp.max(far, axis=-1, keepdims=True),
                        )
                        peak = jnp.maximum(peak, sink)
                        near = jnp.exp(near - peak)
                        far = jnp.exp(far - peak)
                        total = (
                            jnp.sum(near, axis=-1, keepdims=True)
                            + jnp.sum(far, axis=-1, keepdims=True)
                            + jnp.exp(sink - peak)
                        )
                        exps += [near.astype(BF16), far.astype(BF16)]
                        scale.append(1.0 / total)
                    weights = jnp.concatenate(exps, axis=1)
                    result = jnp.dot(weights, v_wide, preferred_element_type=F32)
                    result = result * jnp.where(out_low, scale[0], scale[1])
                    gate = gbuf[rows, cols].astype(F32)
                    gate = gate / (1.0 + jnp.exp(-gate))
                    mixed[:, cols] = (result * gate).astype(BF16)

    def out_copy(c, n):
        return pltpu.make_async_remote_copy(
            src_ref=bsend.at[c, n],
            dst_ref=brecv.at[c, n],
            send_sem=out_sem.at[0, c, n],
            recv_sem=out_sem.at[1, c, n],
            device_id={"tp": other},
            device_id_type=MESH,
        )

    def far_chunk(c, carry):
        attend_rows(pl.multiple_of(far_at + c * Q_ROWS, 16))

        def product(n, inner):
            cols = pl.ds(pl.multiple_of(n * piece, LANES), piece)
            y = jnp.dot(mixed[...], wo[:, cols], preferred_element_type=F32)
            bsend[c, n] = y.astype(BF16)
            out_copy(c, n).start()
            return inner

        lax.fori_loop(0, PIECES, product, 0)
        return carry

    lax.fori_loop(0, chunks_own, far_chunk, 0)

    @pl.when(has_early_to)
    def _():
        early.wait_send()
        late.wait_recv()

    @pl.when(has_late_to)
    def _():
        late.wait_send()

    def own_chunk(c, carry):
        attend_rows(pl.multiple_of(own_at + c * Q_ROWS, 16))

        def product(n, inner):
            cols = pl.ds(pl.multiple_of(n * piece, LANES), piece)
            y = jnp.dot(mixed[...], wo[:, cols], preferred_element_type=F32)
            out_ref[pl.ds(pl.multiple_of(c * Q_ROWS, 16), Q_ROWS), cols] = y.astype(BF16)
            return inner

        lax.fori_loop(0, PIECES, product, 0)
        return carry

    lax.fori_loop(0, chunks_own, own_chunk, 0)

    def finish(s, carry):
        c = s // PIECES
        n = s % PIECES
        out_copy(c, n).wait()
        cols = pl.ds(pl.multiple_of(n * piece, LANES), piece)
        rows = pl.ds(pl.multiple_of(c * Q_ROWS, 16), Q_ROWS)
        lat_at = pl.ds(pl.multiple_of(own_at + c * Q_ROWS, 16), Q_ROWS)
        branch = out_ref[rows, cols].astype(F32) + brecv[c, n].astype(F32)
        moved = lat[lat_at, cols].astype(F32) + modv[4:5, cols] * branch
        out_ref[rows, cols] = moved.astype(BF16)
        return carry

    lax.fori_loop(0, chunks_own * PIECES, finish, 0)


def rotation_tables(sp_rank, block_rows):
    positions = sp_rank * block_rows + jnp.arange(block_rows, dtype=jnp.int32)
    quarter = HEAD_SIZE // 4
    inverse = jnp.exp(-math.log(10000.0) * jnp.arange(quarter, dtype=jnp.float32) / quarter)
    grid_row = (positions // GRID_W).astype(jnp.float32)
    mesh_column = (positions % GRID_W).astype(jnp.float32)
    angles = jnp.concatenate([grid_row[:, None] * inverse, mesh_column[:, None] * inverse], axis=1)
    cosine = jnp.cos(angles)
    sine = jnp.sin(angles)
    copies = LANES // HEAD_SIZE
    return (
        jnp.concatenate([cosine, cosine] * copies, axis=1),
        jnp.concatenate([-sine, sine] * copies, axis=1),
    )


def fused_shards(
    latent,
    condition,
    ctx_condition,
    context,
    mod_shift,
    mod_scale,
    mod_gate,
    norm_gain,
    w_query,
    key_weight,
    value_weight,
    w_gate,
    w_out,
    sink_logit,
):
    sp_count = lax.axis_size("sp")
    rows, width = latent.shape
    block = 2 * rows
    mod_rows, mod_cols = mod_shift.shape
    q_width = w_query.shape[1]
    kv_width = key_weight.shape[1]
    ctx_own = context.shape[0]
    cosine, sine = rotation_tables(lax.axis_index("sp"), block)
    kv_rows = block + 2 * WINDOW
    chunks = rows // Q_ROWS
    piece = width // PIECES
    anywhere = pl.BlockSpec(memory_space=pl.ANY)
    vmem = pl.BlockSpec(memory_space=pltpu.VMEM)
    smem = pl.BlockSpec(memory_space=pltpu.SMEM)
    dma = pltpu.SemaphoreType.DMA
    return pl.pallas_call(
        functools.partial(block_kernel, sp_count),
        out_shape=jax.ShapeDtypeStruct((rows, width), BF16),
        in_specs=[anywhere, vmem, vmem, anywhere, anywhere, anywhere, anywhere, vmem]
        + [anywhere] * 5
        + [smem, vmem, vmem],
        out_specs=vmem,
        scratch_shapes=[
            pltpu.VMEM((block, width), BF16),
            pltpu.VMEM((ctx_own, width), BF16),
            pltpu.VMEM((3, mod_rows, mod_cols), BF16),
            pltpu.VMEM((width, q_width), BF16),
            pltpu.VMEM((width, kv_width), BF16),
            pltpu.VMEM((width, kv_width), BF16),
            pltpu.VMEM((width, q_width), BF16),
            pltpu.VMEM((q_width, width), BF16),
            pltpu.VMEM((8, mod_cols), F32),
            pltpu.VMEM((sp_count - 1, 8, mod_cols), F32),
            pltpu.VMEM((2, 8, mod_cols), F32),
            pltpu.VMEM((8, width), F32),
            pltpu.VMEM((block, width), BF16),
            pltpu.VMEM((ctx_own, width), BF16),
            pltpu.VMEM((block, q_width), BF16),
            pltpu.VMEM((block, q_width), BF16),
            pltpu.VMEM((kv_rows, 2 * kv_width), BF16),
            pltpu.VMEM((ctx_own * sp_count, 2 * kv_width), BF16),
            pltpu.VMEM((Q_ROWS, q_width), BF16),
            pltpu.VMEM((chunks, PIECES, Q_ROWS, piece), BF16),
            pltpu.VMEM((chunks, PIECES, Q_ROWS, piece), BF16),
            dma((10,)),
            dma((2, chunks)),
            dma((2, sp_count - 1)),
            dma((2,)),
            dma((2, sp_count - 1)),
            dma((2, 2)),
            dma((2, chunks, PIECES)),
        ],
        compiler_params=pltpu.CompilerParams(
            collective_id=0, has_side_effects=True, vmem_limit_bytes=62 * 1024 * 1024
        ),
        name="block_kernel",
    )(
        latent,
        condition[None, :],
        ctx_condition[None, :],
        context,
        mod_shift,
        mod_scale,
        mod_gate,
        norm_gain[None, :],
        w_query,
        key_weight,
        value_weight,
        w_gate,
        w_out,
        sink_logit,
        cosine,
        sine,
    )


def solution(mesh):
    return jax.shard_map(
        fused_shards if mesh.shape["tp"] == 2 else shards,
        mesh=mesh,
        in_specs=(
            P(("dp", "sp", "tp"), None),
            P("dp"),
            P(),
            P(("dp", "sp"), None),
            P("sp", "tp"),
            P("sp", "tp"),
            P("sp", "tp"),
            P(),
            P(None, "tp"),
            P(None, "tp"),
            P(None, "tp"),
            P(None, "tp"),
            P("tp", None),
            P("tp"),
        ),
        out_specs=P(("dp", "sp", "tp"), None),
        check_vma=False,
    )
```

```python
import functools
import math

import jax
import jax.numpy as jnp
from jax import lax
from jax.experimental import pallas as pl
from jax.experimental.pallas import tpu as pltpu
from jax.sharding import PartitionSpec as P

HEAD_SIZE = 64
WINDOW = 128
GRID_W = 64


NORM_EPS = 1e-06
MASK_VALUE = -1e30


def with_halo(block, sides, width):
    for axis, dim in sides:
        count = lax.axis_size(axis)
        forward = [(i, i + 1) for i in range(count - 1)]
        backward = [(target, source) for source, target in forward]
        low = lax.ppermute(
            lax.slice_in_dim(block, block.shape[dim] - width, None, axis=dim), axis, forward
        )
        high = lax.ppermute(lax.slice_in_dim(block, 0, width, axis=dim), axis, backward)
        block = jnp.concatenate([low, block, high], axis=dim)
    return block


def modulate(row_data, gain_vec, shift_vec, scale_vec):
    values = row_data.astype(jnp.float32)
    inverse = lax.rsqrt(jnp.mean(values * values, axis=-1, keepdims=True) + NORM_EPS)
    return (values * inverse * gain_vec * (1.0 + scale_vec) + shift_vec).astype(jnp.bfloat16)


def rotate(projected, positions):
    row_count = projected.shape[0]
    head_count = projected.shape[1] // HEAD_SIZE
    quarter = HEAD_SIZE // 4
    half_dim = HEAD_SIZE // 2
    inverse = jnp.exp(-math.log(10000.0) * jnp.arange(quarter, dtype=jnp.float32) / quarter)
    grid_row = (positions // GRID_W).astype(jnp.float32)
    mesh_column = (positions % GRID_W).astype(jnp.float32)
    angles = jnp.concatenate([grid_row[:, None] * inverse, mesh_column[:, None] * inverse], axis=1)
    cosine = jnp.cos(angles)[:, None, :]
    sine_table = jnp.sin(angles)[:, None, :]
    shaped = projected.reshape(row_count, head_count, HEAD_SIZE)
    first_half = shaped[..., :half_dim]
    second = shaped[..., half_dim:]
    turned = jnp.concatenate(
        [first_half * cosine - second * sine_table, second * cosine + first_half * sine_table],
        axis=-1,
    )
    return turned.reshape(row_count, head_count * HEAD_SIZE)


def attend(
    queries, key_rows, value_rows, ctx_keys, ctx_values, sink_logit, q_begin, k_begin, seq_total
):
    row_count = queries.shape[0]
    key_count = key_rows.shape[0]
    ctx_count = ctx_keys.shape[0]
    kv_heads = key_rows.shape[1] // HEAD_SIZE
    head_count = queries.shape[1] // HEAD_SIZE
    group_size = head_count // kv_heads
    factor = 1.0 / math.sqrt(HEAD_SIZE)
    q_heads = queries.reshape(row_count, kv_heads, group_size, HEAD_SIZE)
    k_heads = key_rows.reshape(key_count, kv_heads, HEAD_SIZE)
    v_heads = value_rows.reshape(key_count, kv_heads, HEAD_SIZE)
    ck_heads = ctx_keys.reshape(ctx_count, kv_heads, HEAD_SIZE)
    cv_heads = ctx_values.reshape(ctx_count, kv_heads, HEAD_SIZE)
    near_scores = (
        jnp.einsum("qkgd,skd->kgqs", q_heads, k_heads, preferred_element_type=jnp.float32) * factor
    )
    q_pos = q_begin + jnp.arange(row_count, dtype=jnp.int32)
    k_pos = k_begin + jnp.arange(key_count, dtype=jnp.int32)
    in_window = (jnp.abs(q_pos[:, None] - k_pos[None, :]) <= WINDOW) & (
        (k_pos >= 0) & (k_pos < seq_total)
    )[None, :]
    near_scores = jnp.where(in_window, near_scores, MASK_VALUE)
    ctx_scores = (
        jnp.einsum("qkgd,skd->kgqs", q_heads, ck_heads, preferred_element_type=jnp.float32) * factor
    )
    sink_score = sink_logit.reshape(kv_heads, group_size)[:, :, None, None]
    peak_score = jnp.maximum(
        jnp.maximum(
            jnp.max(near_scores, axis=-1, keepdims=True),
            jnp.max(ctx_scores, axis=-1, keepdims=True),
        ),
        sink_score,
    )
    near_exp = jnp.exp(near_scores - peak_score)
    ctx_exp = jnp.exp(ctx_scores - peak_score)
    softmax_denominator = (
        jnp.sum(near_exp, axis=-1, keepdims=True)
        + jnp.sum(ctx_exp, axis=-1, keepdims=True)
        + jnp.exp(sink_score - peak_score)
    )
    near_weights = (near_exp / softmax_denominator).astype(jnp.bfloat16)
    ctx_weights = (ctx_exp / softmax_denominator).astype(jnp.bfloat16)
    result = jnp.einsum("kgqs,skd->qkgd", near_weights, v_heads, preferred_element_type=jnp.float32)
    result = result + jnp.einsum(
        "kgqs,skd->qkgd", ctx_weights, cv_heads, preferred_element_type=jnp.float32
    )
    return result.reshape(row_count, head_count * HEAD_SIZE)


def shards(
    latent,
    condition,
    ctx_condition,
    context,
    mod_shift,
    mod_scale,
    mod_gate,
    norm_gain,
    w_query,
    key_weight,
    value_weight,
    w_gate,
    w_out,
    sink_logit,
):
    sp_count = lax.axis_size("sp")
    sp_rank = lax.axis_index("sp")
    mod_rows = mod_shift.shape[0]
    cond_act = jax.nn.silu(condition).astype(jnp.bfloat16)
    ctx_act = jax.nn.silu(ctx_condition).astype(jnp.bfloat16)
    first_row = sp_rank * mod_rows
    lat_piece = lax.dynamic_slice_in_dim(cond_act, first_row, mod_rows, 0)
    ctx_piece = lax.dynamic_slice_in_dim(ctx_act, first_row, mod_rows, 0)
    both_conds = jnp.stack([lat_piece, ctx_piece])
    partial_value = jnp.concatenate(
        [
            jnp.dot(both_conds, mod_shift, preferred_element_type=jnp.float32),
            jnp.dot(both_conds, mod_scale, preferred_element_type=jnp.float32),
            jnp.dot(lat_piece[None, :], mod_gate, preferred_element_type=jnp.float32),
        ],
        axis=0,
    )
    summed = lax.psum(partial_value, "sp")
    vectors = lax.all_gather(summed, "tp", axis=1, tiled=True)
    lat_shift = vectors[0]
    ctx_shift = vectors[1]
    lat_scale = vectors[2]
    ctx_scale = vectors[3]
    lat_gate = vectors[4]
    hidden = modulate(latent, norm_gain, lat_shift, lat_scale)
    ctx_hidden = modulate(context, norm_gain, ctx_shift, ctx_scale)
    kv_width = key_weight.shape[1]
    q_width = w_query.shape[1]
    ctx_pair = jnp.concatenate(
        [
            jnp.dot(ctx_hidden, key_weight, preferred_element_type=jnp.float32).astype(
                jnp.bfloat16
            ),
            jnp.dot(ctx_hidden, value_weight, preferred_element_type=jnp.float32).astype(
                jnp.bfloat16
            ),
        ],
        axis=1,
    )
    ctx_all = lax.all_gather(ctx_pair, "sp", axis=0, tiled=True)
    row_piece = lax.all_gather(hidden, "tp", axis=0, tiled=True)
    projected = jnp.concatenate(
        [
            jnp.dot(row_piece, w_query, preferred_element_type=jnp.float32),
            jnp.dot(row_piece, key_weight, preferred_element_type=jnp.float32),
            jnp.dot(row_piece, value_weight, preferred_element_type=jnp.float32),
            jnp.dot(row_piece, w_gate, preferred_element_type=jnp.float32),
        ],
        axis=1,
    )
    block_rows = projected.shape[0]
    q_begin = sp_rank * block_rows
    positions = q_begin + jnp.arange(block_rows, dtype=jnp.int32)
    queries = rotate(projected[:, :q_width], positions).astype(jnp.bfloat16)
    key_rows = rotate(projected[:, q_width : q_width + kv_width], positions).astype(jnp.bfloat16)
    value_rows = projected[:, q_width + kv_width : q_width + 2 * kv_width].astype(jnp.bfloat16)
    gate_proj = projected[:, q_width + 2 * kv_width :].astype(jnp.bfloat16)
    key_value = jnp.concatenate([key_rows, value_rows], axis=1)
    padded = with_halo(key_value, (("sp", 0),), WINDOW)
    attended = attend(
        queries,
        padded[:, :kv_width],
        padded[:, kv_width:],
        ctx_all[:, :kv_width],
        ctx_all[:, kv_width:],
        sink_logit,
        q_begin,
        q_begin - WINDOW,
        block_rows * sp_count,
    )
    mixed = (attended * jax.nn.silu(gate_proj.astype(jnp.float32))).astype(jnp.bfloat16)
    branch = lax.psum_scatter(
        jnp.dot(mixed, w_out, preferred_element_type=jnp.float32).astype(jnp.bfloat16),
        "tp",
        scatter_dimension=0,
        tiled=True,
    ).astype(jnp.float32)
    return (latent.astype(jnp.float32) + lat_gate * branch).astype(jnp.bfloat16)


MESH = pl.DeviceIdType.MESH
LANES = 128
Q_ROWS = 80
PIECES = 4
F32 = jnp.float32
BF16 = jnp.bfloat16


def block_kernel(
    sp_count,
    latent_hbm,
    cond_ref,
    ctx_cond_ref,
    context_hbm,
    ms_hbm,
    mc_hbm,
    mg_hbm,
    gain_ref,
    wq_hbm,
    wk_hbm,
    wv_hbm,
    wg_hbm,
    wo_hbm,
    sink_ref,
    out_hbm,
    out_ref,
    cos_ref,
    sin_ref,
    lat,
    ctx_rows,
    mods,
    wq,
    wk,
    wv,
    wg,
    wo,
    part,
    part_in,
    vecs,
    modv,
    hid,
    ctx_hid,
    qbuf,
    gbuf,
    kv,
    ctx_kv,
    mixed,
    bsend,
    brecv,
    local_sem,
    lat_sem,
    part_sem,
    vec_sem,
    ctx_sem,
    halo_sem,
    out_sem,
    store_sem,
):
    rank = lax.axis_index("sp")
    side = lax.axis_index("tp")
    other = 1 - side
    own_rows, width = latent_hbm.shape
    block = 2 * own_rows
    mod_rows, mod_cols = ms_hbm.shape
    kv_width = wk.shape[1]
    q_width = wq.shape[1]
    ctx_own = context_hbm.shape[0]
    ctx_total = ctx_own * sp_count
    kv_heads = kv_width // HEAD_SIZE
    pairs = q_width // LANES // kv_heads
    keys = Q_ROWS + 2 * WINDOW
    span = -(-keys // LANES) * LANES
    total_keys = span + ctx_total
    piece = width // PIECES
    chunks_own = own_rows // Q_ROWS
    low_end = WINDOW + block

    def load(src, dst, index):
        return pltpu.make_async_copy(src, dst, local_sem.at[index])

    own_at = pl.multiple_of(side * own_rows, 16)
    far_at = pl.multiple_of(other * own_rows, 16)
    loads = [
        load(ms_hbm, mods.at[0], 0),
        load(mc_hbm, mods.at[1], 1),
        load(mg_hbm, mods.at[2], 2),
        load(latent_hbm, lat.at[pl.ds(own_at, own_rows)], 3),
        load(context_hbm, ctx_rows, 4),
        load(wk_hbm, wk, 5),
        load(wv_hbm, wv, 6),
        load(wq_hbm, wq, 7),
        load(wg_hbm, wg, 8),
        load(wo_hbm, wo, 9),
    ]
    for copy in loads[0:5]:
        copy.start()

    barrier = pltpu.get_barrier_semaphore()
    pl.semaphore_signal(barrier, inc=1, device_id={"tp": other}, device_id_type=MESH)
    for step in range(1, sp_count):
        peer = lax.rem(rank + step, sp_count)
        pl.semaphore_signal(barrier, inc=1, device_id={"sp": peer}, device_id_type=MESH)
    pl.semaphore_wait(barrier, sp_count)

    def lat_copy(c):
        return pltpu.make_async_remote_copy(
            src_ref=latent_hbm.at[pl.ds(c * Q_ROWS, Q_ROWS)],
            dst_ref=lat.at[pl.ds(pl.multiple_of(own_at + c * Q_ROWS, 16), Q_ROWS)],
            send_sem=lat_sem.at[0, c],
            recv_sem=lat_sem.at[1, c],
            device_id={"tp": other},
            device_id_type=MESH,
        )

    lat_copies = [lat_copy(c) for c in range(chunks_own)]
    lat_copies[0].start()

    @pl.when(rank == 0)
    def _():
        kv[0:WINDOW, :] = jnp.zeros((WINDOW, 2 * kv_width), BF16)

    @pl.when(rank == sp_count - 1)
    def _():
        kv[low_end : low_end + WINDOW, :] = jnp.zeros((WINDOW, 2 * kv_width), BF16)

    first = pl.multiple_of(rank * mod_rows, LANES)
    lat_c = cond_ref[:, pl.ds(first, mod_rows)]
    ctx_c = ctx_cond_ref[:, pl.ds(first, mod_rows)]
    row_id = lax.broadcasted_iota(jnp.int32, (16, mod_rows), 0)
    both = jnp.where(row_id == 0, lat_c, ctx_c)
    both = (both / (1.0 + jnp.exp(-both))).astype(BF16)
    tile = mod_cols // 3
    for m in range(3):
        loads[m].wait()
        for t in range(3):
            cols = slice(t * tile, (t + 1) * tile)
            prod = jnp.dot(both, mods[m, :, cols], preferred_element_type=F32)
            part[2 * m : 2 * m + 2, cols] = prod[0:2, :]
    for copy in loads[5:]:
        copy.start()
    part[6:8, :] = jnp.zeros((2, mod_cols), F32)

    part_copies = []
    for step in range(1, sp_count):
        peer = lax.rem(rank + step, sp_count)
        copy = pltpu.make_async_remote_copy(
            src_ref=part,
            dst_ref=part_in.at[step - 1],
            send_sem=part_sem.at[0, step - 1],
            recv_sem=part_sem.at[1, step - 1],
            device_id={"sp": peer},
            device_id_type=MESH,
        )
        copy.start()
        part_copies.append(copy)

    def table_rows(g, carry):
        rows = pl.ds(pl.multiple_of(g * 32, 32), 32)
        lane = lax.broadcasted_iota(jnp.int32, (32, LANES), 1)
        position = rank * block + g * 32 + lax.broadcasted_iota(jnp.int32, (32, LANES), 0)
        quarter = HEAD_SIZE // 4
        inverse = jnp.exp(-math.log(10000.0) * (lane % quarter).astype(F32) / quarter)
        in_row = lane % (2 * quarter) < quarter
        place = jnp.where(in_row, position // GRID_W, position % GRID_W).astype(F32)
        angles = place * inverse
        cos_ref[rows, :] = jnp.cos(angles)
        sine = jnp.sin(angles)
        sin_ref[rows, :] = jnp.where(lane % HEAD_SIZE < 2 * quarter, -sine, sine)
        return carry

    lax.fori_loop(0, block // 32, table_rows, 0)
    for copy in part_copies:
        copy.wait()
    summed = part[...]
    for step in range(sp_count - 1):
        summed = summed + part_in[step]
    vecs[side] = summed
    vec_copy = pltpu.make_async_remote_copy(
        src_ref=vecs.at[side],
        dst_ref=vecs.at[side],
        send_sem=vec_sem.at[0],
        recv_sem=vec_sem.at[1],
        device_id={"tp": other},
        device_id_type=MESH,
    )
    vec_copy.start()
    for copy in lat_copies[1:]:
        copy.start()
    vec_copy.wait()
    for h in range(2):
        cols = slice(h * mod_cols, (h + 1) * mod_cols)
        gain = gain_ref[:, cols]
        modv[0:1, cols] = gain * (1.0 + vecs[h, 2:3, :])
        modv[1:2, cols] = vecs[h, 0:1, :]
        modv[2:3, cols] = gain * (1.0 + vecs[h, 3:4, :])
        modv[3:4, cols] = vecs[h, 1:2, :]
        modv[4:5, cols] = vecs[h, 4:5, :]

    def modulate_rows(src, dst, begin, count, which):
        def body(i, carry):
            rows = pl.ds(pl.multiple_of(begin + i * 16, 16), 16)
            values = src[rows, :].astype(F32)
            mean = jnp.sum(values * values, axis=-1, keepdims=True) * (1.0 / width)
            inverse = lax.rsqrt(mean + NORM_EPS)
            scaled = values * inverse * modv[which : which + 1, :] + modv[which + 1 : which + 2, :]
            dst[rows, :] = scaled.astype(BF16)
            return carry

        lax.fori_loop(0, count // 16, body, 0)

    def turn(values, rows, factor):
        lane = lax.broadcasted_iota(jnp.int32, values.shape, 1)
        half = HEAD_SIZE // 2
        ahead = pltpu.roll(values, LANES - half, 1)
        behind = pltpu.roll(values, half, 1)
        swapped = jnp.where(lane % HEAD_SIZE < half, ahead, behind)
        turned = values * cos_ref[rows, :] + swapped * sin_ref[rows, :]
        return turned * factor

    def project_kv(begin, count):
        rows = pl.ds(begin, count)
        into = pl.ds(pl.multiple_of(begin + WINDOW, 16), count)
        x = hid[rows, :]
        k = jnp.dot(x, wk[...], preferred_element_type=F32)
        for c in range(kv_width // LANES):
            cols = slice(c * LANES, (c + 1) * LANES)
            kv[into, cols] = turn(k[:, cols], rows, 1.0).astype(BF16)
        v = jnp.dot(x, wv[...], preferred_element_type=F32)
        kv[into, kv_width : 2 * kv_width] = v.astype(BF16)

    step_cols = 2 * LANES

    def project_q(begin, count):
        rows = pl.ds(begin, count)
        factor = 1.0 / math.sqrt(HEAD_SIZE)

        def body(t, carry):
            at = pl.multiple_of(t * step_cols, step_cols)
            y = jnp.dot(hid[rows, :], wq[:, pl.ds(at, step_cols)], preferred_element_type=F32)
            for c in range(2):
                cols = pl.ds(pl.multiple_of(at + c * LANES, LANES), LANES)
                part_y = y[:, c * LANES : (c + 1) * LANES]
                qbuf[rows, cols] = turn(part_y, rows, factor).astype(BF16)
            return carry

        lax.fori_loop(0, q_width // step_cols, body, 0)

    def project_g(begin, count):
        rows = pl.ds(begin, count)

        def body(t, carry):
            cols = pl.ds(pl.multiple_of(t * step_cols, step_cols), step_cols)
            y = jnp.dot(hid[rows, :], wg[:, cols], preferred_element_type=F32)
            gbuf[rows, cols] = y.astype(BF16)
            return carry

        lax.fori_loop(0, q_width // step_cols, body, 0)

    loads[4].wait()
    modulate_rows(ctx_rows, ctx_hid, 0, ctx_own, 2)
    loads[5].wait()
    loads[6].wait()
    ctx_at = pl.ds(pl.multiple_of(rank * ctx_own, 16), ctx_own)
    xc = ctx_hid[...]
    ctx_kv[ctx_at, 0:kv_width] = jnp.dot(xc, wk[...], preferred_element_type=F32).astype(BF16)
    ctx_kv[ctx_at, kv_width : 2 * kv_width] = jnp.dot(
        xc, wv[...], preferred_element_type=F32
    ).astype(BF16)
    ctx_copies = []
    for step in range(1, sp_count):
        peer = lax.rem(rank + step, sp_count)
        copy = pltpu.make_async_remote_copy(
            src_ref=ctx_kv.at[ctx_at],
            dst_ref=ctx_kv.at[ctx_at],
            send_sem=ctx_sem.at[0, step - 1],
            recv_sem=ctx_sem.at[1, step - 1],
            device_id={"sp": peer},
            device_id_type=MESH,
        )
        copy.start()
        ctx_copies.append(copy)

    def halo(src_at, dst_at, index, target):
        return pltpu.make_async_remote_copy(
            src_ref=kv.at[pl.ds(pl.multiple_of(src_at, 16), WINDOW)],
            dst_ref=kv.at[pl.ds(pl.multiple_of(dst_at, 16), WINDOW)],
            send_sem=halo_sem.at[0, index],
            recv_sem=halo_sem.at[1, index],
            device_id={"sp": target},
            device_id_type=MESH,
        )

    early_to = rank - 1 + 2 * side
    late_to = rank + 1 - 2 * side
    has_early_to = (early_to >= 0) & (early_to < sp_count)
    has_late_to = (late_to >= 0) & (late_to < sp_count)
    early = halo(WINDOW + side * (block - WINDOW), other * low_end, 0, early_to)
    late = halo(WINDOW + other * (block - WINDOW), side * low_end, 1, late_to)

    loads[3].wait()
    modulate_rows(lat, hid, own_at, own_rows, 0)
    project_kv(own_at, own_rows)

    @pl.when(has_early_to)
    def _():
        early.start()

    for c in range(chunks_own):
        chunk_at = pl.multiple_of(far_at + c * Q_ROWS, 16)
        lat_copies[c].wait()
        modulate_rows(lat, hid, chunk_at, Q_ROWS, 0)
        project_kv(chunk_at, Q_ROWS)
        if c == 0:
            loads[7].wait()
            project_q(chunk_at, Q_ROWS)
            loads[8].wait()
            project_g(chunk_at, Q_ROWS)

    @pl.when(has_late_to)
    def _():
        late.start()

    for copy in ctx_copies:
        copy.wait()

    @pl.when(has_late_to)
    def _():
        early.wait_recv()

    loads[9].wait()

    def attend_rows(begin):
        rows = pl.ds(begin, Q_ROWS)
        i = lax.broadcasted_iota(jnp.int32, (Q_ROWS, span), 0)
        j = lax.broadcasted_iota(jnp.int32, (Q_ROWS, span), 1)
        offset = j - i
        k_pos = rank * block + begin - WINDOW + j
        allowed = (offset >= 0) & (offset <= 2 * WINDOW) & (k_pos >= 0)
        allowed = allowed & (k_pos < block * sp_count)
        bias = jnp.where(allowed, 0.0, MASK_VALUE)
        lane = lax.broadcasted_iota(jnp.int32, (total_keys, LANES), 1)
        low_lane = lane < HEAD_SIZE
        filler = jnp.zeros((span - keys, LANES), BF16)
        out_low = lax.broadcasted_iota(jnp.int32, (Q_ROWS, LANES), 1) < HEAD_SIZE

        def both_heads(at):
            cols = slice(at, at + LANES)
            tile_kv = jnp.concatenate(
                [kv[pl.ds(begin, keys), cols], filler, ctx_kv[:, cols]], axis=0
            ).astype(F32)
            turned = pltpu.roll(tile_kv, HEAD_SIZE, 1)
            even = jnp.concatenate(
                [jnp.where(low_lane, tile_kv, 0.0), jnp.where(low_lane, 0.0, turned)], axis=0
            )
            odd = jnp.concatenate(
                [jnp.where(low_lane, turned, 0.0), jnp.where(low_lane, 0.0, tile_kv)], axis=0
            )
            return even.astype(BF16), odd.astype(BF16)

        for tile_id in range(kv_heads // 2):
            k_two = both_heads(tile_id * LANES)
            v_two = both_heads(kv_width + tile_id * LANES)
            for parity in range(2):
                head = 2 * tile_id + parity
                k_wide = k_two[parity]
                v_wide = v_two[parity]
                base = head * pairs
                for p in range(pairs):
                    cols = slice((base + p) * LANES, (base + p + 1) * LANES)
                    scores = lax.dot_general(
                        qbuf[rows, cols],
                        k_wide,
                        (((1,), (1,)), ((), ())),
                        preferred_element_type=F32,
                    )
                    exps = []
                    scale = []
                    for h in range(2):
                        sink = sink_ref[2 * (base + p) + h]
                        near = scores[:, h * total_keys : h * total_keys + span] + bias
                        far = scores[:, h * total_keys + span : (h + 1) * total_keys]
                        peak = jnp.maximum(
                            jnp.max(near, axis=-1, keepdims=True),
                            jnp.max(far, axis=-1, keepdims=True),
                        )
                        peak = jnp.maximum(peak, sink)
                        near = jnp.exp(near - peak)
                        far = jnp.exp(far - peak)
                        total = (
                            jnp.sum(near, axis=-1, keepdims=True)
                            + jnp.sum(far, axis=-1, keepdims=True)
                            + jnp.exp(sink - peak)
                        )
                        exps += [near.astype(BF16), far.astype(BF16)]
                        scale.append(1.0 / total)
                    weights = jnp.concatenate(exps, axis=1)
                    result = jnp.dot(weights, v_wide, preferred_element_type=F32)
                    result = result * jnp.where(out_low, scale[0], scale[1])
                    gate = gbuf[rows, cols].astype(F32)
                    gate = gate / (1.0 + jnp.exp(-gate))
                    mixed[:, cols] = (result * gate).astype(BF16)

    def out_copy(c, n):
        return pltpu.make_async_remote_copy(
            src_ref=bsend.at[c, n],
            dst_ref=brecv.at[c, n],
            send_sem=out_sem.at[0, c, n],
            recv_sem=out_sem.at[1, c, n],
            device_id={"tp": other},
            device_id_type=MESH,
        )

    def far_chunk(c, carry):
        chunk_at = pl.multiple_of(far_at + c * Q_ROWS, 16)

        @pl.when(c > 0)
        def _():
            project_q(chunk_at, Q_ROWS)
            project_g(chunk_at, Q_ROWS)

        attend_rows(chunk_at)

        def product(n, inner):
            cols = pl.ds(pl.multiple_of(n * piece, LANES), piece)
            y = jnp.dot(mixed[...], wo[:, cols], preferred_element_type=F32)
            bsend[c, n] = y.astype(BF16)
            out_copy(c, n).start()
            return inner

        lax.fori_loop(0, PIECES, product, 0)
        return carry

    lax.fori_loop(0, chunks_own, far_chunk, 0)
    project_q(own_at, own_rows)
    project_g(own_at, own_rows)

    @pl.when(has_early_to)
    def _():
        early.wait_send()
        late.wait_recv()

    @pl.when(has_late_to)
    def _():
        late.wait_send()

    def own_chunk(c, carry):
        attend_rows(pl.multiple_of(own_at + c * Q_ROWS, 16))

        def product(n, inner):
            cols = pl.ds(pl.multiple_of(n * piece, LANES), piece)
            y = jnp.dot(mixed[...], wo[:, cols], preferred_element_type=F32)
            out_ref[pl.ds(pl.multiple_of(c * Q_ROWS, 16), Q_ROWS), cols] = y.astype(BF16)
            return inner

        lax.fori_loop(0, PIECES, product, 0)
        return carry

    lax.fori_loop(0, chunks_own, own_chunk, 0)

    def store(c, n):
        cols = pl.ds(pl.multiple_of(n * piece, LANES), piece)
        rows = pl.ds(pl.multiple_of(c * Q_ROWS, 16), Q_ROWS)
        return pltpu.make_async_copy(
            out_ref.at[rows, cols], out_hbm.at[rows, cols], store_sem.at[c, n]
        )

    def finish(s, carry):
        c = s // PIECES
        n = s % PIECES
        out_copy(c, n).wait()
        cols = pl.ds(pl.multiple_of(n * piece, LANES), piece)
        rows = pl.ds(pl.multiple_of(c * Q_ROWS, 16), Q_ROWS)
        lat_at = pl.ds(pl.multiple_of(own_at + c * Q_ROWS, 16), Q_ROWS)
        branch = out_ref[rows, cols].astype(F32) + brecv[c, n].astype(F32)
        moved = lat[lat_at, cols].astype(F32) + modv[4:5, cols] * branch
        out_ref[rows, cols] = moved.astype(BF16)
        store(c, n).start()
        return carry

    lax.fori_loop(0, chunks_own * PIECES, finish, 0)
    for c in range(chunks_own):
        for n in range(PIECES):
            store(c, n).wait()


def fused_shards(
    latent,
    condition,
    ctx_condition,
    context,
    mod_shift,
    mod_scale,
    mod_gate,
    norm_gain,
    w_query,
    key_weight,
    value_weight,
    w_gate,
    w_out,
    sink_logit,
):
    sp_count = lax.axis_size("sp")
    rows, width = latent.shape
    block = 2 * rows
    mod_rows, mod_cols = mod_shift.shape
    q_width = w_query.shape[1]
    kv_width = key_weight.shape[1]
    ctx_own = context.shape[0]
    kv_rows = block + 2 * WINDOW
    chunks = rows // Q_ROWS
    piece = width // PIECES
    anywhere = pl.BlockSpec(memory_space=pl.ANY)
    vmem = pl.BlockSpec(memory_space=pltpu.VMEM)
    smem = pl.BlockSpec(memory_space=pltpu.SMEM)
    dma = pltpu.SemaphoreType.DMA
    return pl.pallas_call(
        functools.partial(block_kernel, sp_count),
        out_shape=jax.ShapeDtypeStruct((rows, width), BF16),
        in_specs=[anywhere, vmem, vmem, anywhere, anywhere, anywhere, anywhere, vmem]
        + [anywhere] * 5
        + [smem],
        out_specs=anywhere,
        scratch_shapes=[
            pltpu.VMEM((rows, width), BF16),
            pltpu.VMEM((block, LANES), F32),
            pltpu.VMEM((block, LANES), F32),
            pltpu.VMEM((block, width), BF16),
            pltpu.VMEM((ctx_own, width), BF16),
            pltpu.VMEM((3, mod_rows, mod_cols), BF16),
            pltpu.VMEM((width, q_width), BF16),
            pltpu.VMEM((width, kv_width), BF16),
            pltpu.VMEM((width, kv_width), BF16),
            pltpu.VMEM((width, q_width), BF16),
            pltpu.VMEM((q_width, width), BF16),
            pltpu.VMEM((8, mod_cols), F32),
            pltpu.VMEM((sp_count - 1, 8, mod_cols), F32),
            pltpu.VMEM((2, 8, mod_cols), F32),
            pltpu.VMEM((8, width), F32),
            pltpu.VMEM((block, width), BF16),
            pltpu.VMEM((ctx_own, width), BF16),
            pltpu.VMEM((block, q_width), BF16),
            pltpu.VMEM((block, q_width), BF16),
            pltpu.VMEM((kv_rows, 2 * kv_width), BF16),
            pltpu.VMEM((ctx_own * sp_count, 2 * kv_width), BF16),
            pltpu.VMEM((Q_ROWS, q_width), BF16),
            pltpu.VMEM((chunks, PIECES, Q_ROWS, piece), BF16),
            pltpu.VMEM((chunks, PIECES, Q_ROWS, piece), BF16),
            dma((10,)),
            dma((2, chunks)),
            dma((2, sp_count - 1)),
            dma((2,)),
            dma((2, sp_count - 1)),
            dma((2, 2)),
            dma((2, chunks, PIECES)),
            dma((chunks, PIECES)),
        ],
        compiler_params=pltpu.CompilerParams(
            collective_id=0, has_side_effects=True, vmem_limit_bytes=62 * 1024 * 1024
        ),
        name="block_kernel",
    )(
        latent,
        condition[None, :],
        ctx_condition[None, :],
        context,
        mod_shift,
        mod_scale,
        mod_gate,
        norm_gain[None, :],
        w_query,
        key_weight,
        value_weight,
        w_gate,
        w_out,
        sink_logit,
    )


def solution(mesh):
    return jax.shard_map(
        fused_shards if mesh.shape["tp"] == 2 else shards,
        mesh=mesh,
        in_specs=(
            P(("dp", "sp", "tp"), None),
            P("dp"),
            P(),
            P(("dp", "sp"), None),
            P("sp", "tp"),
            P("sp", "tp"),
            P("sp", "tp"),
            P(),
            P(None, "tp"),
            P(None, "tp"),
            P(None, "tp"),
            P(None, "tp"),
            P("tp", None),
            P("tp"),
        ),
        out_specs=P(("dp", "sp", "tp"), None),
        check_vma=False,
    )
```
